32 devices in a mesh: grp: 2 (over x), ep: 4 (over y, core), tp: 4 (over z).
Axes of the slice: x: 2, y: 2, z: 4, core: 2. Of those that a mesh axis runs over, the one named last changes fastest.
Arguments:
- tokens: bfloat16 [512, 2048], P(('grp', 'ep')), parts along dimension 0, may hold values from -6 to 6
- routing: int32 [512, 4], P(('grp', 'ep')), parts along dimension 0, may hold values from 0 to 7, all different within a row; in each aligned block of 64 rows (0 to 63, 64 to 127, ...) at most 64 rows name the same one
- route_weight: float32 [512, 4], P(('grp', 'ep')), parts along dimension 0, may hold values from 0.1 to 1
- norm_gain: float32 [2048], replicated, may hold values from 0.1 to 1.9
- gate_weight: bfloat16 [8, 2048, 2048], P('ep', None, 'tp'), may hold values from -2.1213203 to 2.1213203
- up_weight: bfloat16 [8, 2048, 2048], P('ep', None, 'tp'), may hold values from -2.1213203 to 2.1213203
- down_weight: bfloat16 [8, 2048, 2048], P('ep', 'tp'), may hold values from -3.9774756 to 3.9774756
- out_gain: float32 [2048], P('tp'), may hold values from 0.1 to 1.9
Outputs:
- layer_output: bfloat16 [512, 2048], P(('grp', 'ep'), 'tp'), parts along dimension 0
The draws below stay inside these ranges and needn't reach their ends.
There are 2 independent parts, one for each index of `grp`. The reference program is written for one: setup_inputs(seed, part) draws one part's arguments, and reference() takes and returns one part's arrays. A program takes and returns all parts, laid end to end along the dimension named above; an argument that names none is the same for every part. Nothing has to cross between parts.
Inputs may be any that keep to these rules, and one draw needn't show every extreme that they name: `routing`: each row names 4 different experts; among the 64 rows of one index of ep no expert is named more than 64 times, and in some such blocks one expert is named exactly 64 times.
All inputs are finite; a program needn't handle non-finite values.
Results may differ from the reference program's by a relative error of at most 0.017.
Values may be sent and summed in bfloat16 or wider, within the bound.
No kernel may reach another device: no remote copies, remote signals or barrier semaphores. Data moves between devices by JAX's collectives and lax.ppermute only.
A program may use at most 64 MiB of HBM per device.

```python
import math
import jax
import jax.numpy as jnp
import numpy as np
from jax import lax

D = 2048
FF = 2048
TOPK = 4
TOK_DEV = 64
EXPERTS = 8
TOKENS = 256
CAP = 64
EXPERT_ROWS = 256
FF_DEV = 512
N_EP = 4
N_TP = 4


def projection_draw(key, salt_value):
    base = jax.random.fold_in(key, salt_value)
    entry_key, column_key = jax.random.split(base, 2)
    entries = jax.random.truncated_normal(entry_key, -6.0, 6.0, (EXPERTS, D, FF), jnp.float32)
    column = jnp.exp(jax.random.uniform(column_key, (EXPERTS, 1, FF), jnp.float32, 0.0, math.log(8.0)))
    return (entries * column * D ** (-0.5)).astype(jnp.bfloat16)


def draw_gate_weight(key, part):
    return projection_draw(key, 101)


def draw_up_weight(key, part):
    return projection_draw(key, 202)


def draw_down_weight(key, part):
    base = jax.random.fold_in(key, 303)
    entry_key, column_key = jax.random.split(base, 2)
    ramp = jnp.arange(D, dtype=jnp.float32) / D
    entries = jax.random.truncated_normal(entry_key, -6.0, 6.0, (EXPERTS, FF, D), jnp.float32)
    rising = jnp.exp(math.log(4.0) * ramp)
    column = rising[None, None, :] * jnp.exp(jax.random.uniform(column_key, (EXPERTS, 1, D), jnp.float32, 0.0, math.log(3.0)))
    return (entries * column * FF ** (-0.5)).astype(jnp.bfloat16)


def block_levels(rng, extent, cuts, low, largest):
    loudness, own = 1.0, jax.random.fold_in(rng, 6)
    for dim, blocks in cuts:
        heights = jnp.exp(jax.random.uniform(jax.random.fold_in(own, dim), (blocks,), jnp.float32, low / len(cuts), largest / len(cuts)))
        loudness = loudness * jnp.repeat(heights, extent[dim] // blocks).reshape([-1 if axis == dim else 1 for axis in range(len(extent))])
    return loudness


def assign_block(stream_key, own, number, rows, count, top, bound, slope):
    sequence = jax.random.permutation(stream_key, count)
    crowded, usual = shares(count, rows * top, bound, slope, True), shares(count, rows * top, bound, slope, False)
    places = jnp.arange(count)

    def named(lengths, rotation):
        used = int((lengths > 0).sum())
        fixed = max(1, used // 4)
        moved = fixed + (places - fixed + rotation * (used - fixed)) % max(1, count - fixed)
        return jnp.zeros((count,), jnp.int32).at[sequence[jnp.where(places < fixed, places, moved)]].set(jnp.asarray(lengths, jnp.int32))

    lengths = jnp.where(number % 4 == 0, named(crowded, number // 4), named(usual, number - number // 4 - 1))
    mixed = jax.random.permutation(jax.random.fold_in(own, 3), count)
    giver, receiver = mixed[0:count // 2 * 2:2], mixed[1:count // 2 * 2:2]
    margin = jnp.minimum(lengths[giver] - 1, bound - lengths[receiver]) // 2
    margin = jnp.where((giver == sequence[0]) | (receiver == sequence[0]) | (lengths[receiver] == 0), 0, jnp.maximum(margin, 0))
    moved = jax.random.randint(jax.random.fold_in(own, 4), (count // 2,), 0, 1 << 20) % (margin + 1)
    lengths = lengths.at[giver].add(-moved).at[receiver].add(moved)
    members = jnp.searchsorted(jnp.cumsum(lengths), jnp.arange(rows * top), side="right").astype(jnp.int32)
    table = members.reshape(top, rows).T
    table = table[jax.random.permutation(jax.random.fold_in(own, 1), rows)]
    rotation = jax.random.randint(jax.random.fold_in(own, 2), (rows, 1), 0, top)
    return jnp.take_along_axis(table, (jnp.arange(top)[None, :] + rotation) % top, axis=1)


def shares(number_of, total, most, slope, full):
    portions = [(1 << 20) // math.isqrt(rank ** slope) + 1 for rank in range(1, number_of + 1)]
    largest = most if full else min(most, max(-(-total // number_of), total * portions[0] // sum(portions)))
    least = 1 if total - largest >= number_of - 1 else 0
    given, surplus = [largest] + [least] * (number_of - 1), total - largest - least * (number_of - 1)
    while surplus > 0:
        movable = [i for i in range(1, number_of) if given[i] < largest] or [i for i in range(1, number_of) if given[i] < most]
        pool, remaining = sum([portions[i] for i in movable]), surplus
        for i in movable:
            extra = min(most - given[i], max(1, remaining * portions[i] // pool), surplus)
            given[i] = given[i] + extra
            surplus = surplus - extra
    return np.array(given)


def gaussian(own_key, extent, scale, most, shards=(), kind=jnp.bfloat16):
    drawn = scale * jax.random.normal(own_key, extent, jnp.float32)
    if shards:
        drawn = drawn * block_levels(own_key, extent, shards, -0.22, 0.18)
    return jnp.clip(drawn, -most, most).astype(kind)


def setup_inputs(seed: int = 0, part: int = 0) -> dict:
    seeds = jax.random.split(jax.random.key(seed), 9)
    part_splits = jax.random.split(jax.random.fold_in(seeds[8], part), 9)
    tokens = gaussian(part_splits[0], (TOKENS, D), 1.0, 6.0, ((0, 4),))
    routing_keys = jax.random.split(jax.random.fold_in(part_splits[1], 1), TOKENS // TOK_DEV)
    routing_turns = jax.random.permutation(jax.random.fold_in(part_splits[1], 3), TOKENS // TOK_DEV)
    routing = jax.vmap(lambda own, number: assign_block(jax.random.fold_in(part_splits[1], 2), own, number, TOK_DEV, EXPERTS, TOPK, CAP, 2))(routing_keys, routing_turns).reshape((TOKENS, TOPK))
    route_weight = jnp.clip(jnp.exp(math.log(1.0) - 2.3025851 * jax.random.uniform(part_splits[2], (TOKENS, TOPK), jnp.float32) ** block_levels(part_splits[2], (TOKENS, TOPK), ((0, 4),), -0.2, 0.2)), 0.1, 1.0)
    norm_gain = jnp.clip(1.0 + 0.18 * jax.random.normal(seeds[3], (D,), jnp.float32), 0.1, 1.9)
    gate_weight = draw_gate_weight(jax.random.fold_in(seeds[8], 71), part)
    up_weight = draw_up_weight(jax.random.fold_in(seeds[8], 71), part)
    down_weight = draw_down_weight(jax.random.fold_in(seeds[8], 71), part)
    out_gain = jnp.clip(1.0 + 0.18 * jax.random.normal(seeds[7], (D,), jnp.float32), 0.1, 1.9)
    return {"tokens": tokens, "routing": routing, "route_weight": route_weight, "norm_gain": norm_gain, "gate_weight": gate_weight, "up_weight": up_weight, "down_weight": down_weight, "out_gain": out_gain}


LIMIT = 7.0
ALPHA = 1.702
EPS = 1e-06

def slot_ranks(routing):
    assign_count = TOK_DEV * TOPK
    blocks = routing.reshape(N_EP, assign_count)
    same_expert = blocks[:, :, None] == blocks[:, None, :]
    position = jnp.arange(assign_count, dtype=jnp.int32)
    earlier = position[None, :] < position[:, None]
    counted = jnp.where(same_expert & earlier[None, :, :], 1, 0).astype(jnp.int32)
    return lax.optimization_barrier(jnp.sum(counted, axis=2)).astype(jnp.int32).reshape(TOKENS, TOPK)

def reference(tokens, routing, route_weight, norm_gain, gate_weight, up_weight, down_weight, out_gain):
    scaled = tokens.astype(jnp.float32)
    normed = (scaled * lax.rsqrt(lax.optimization_barrier(jnp.mean(scaled * scaled, axis=-1, keepdims=True)) + EPS) * norm_gain).astype(jnp.bfloat16)
    slot_rank = slot_ranks(routing)
    source = (jnp.arange(TOKENS, dtype=jnp.int32) // TOK_DEV)[:, None]
    buffer_row = (source * CAP + slot_rank).astype(jnp.int32)
    buffer = jnp.zeros((EXPERTS, EXPERT_ROWS, D), jnp.bfloat16)
    repeated = jnp.broadcast_to(normed[:, None, :], (TOKENS, TOPK, D))
    buffer = buffer.at[routing, buffer_row].set(repeated)

    def expert(operands):
        expert_rows, gate_block, up_block, down_block = operands
        gate_act = jnp.minimum(jnp.dot(expert_rows, gate_block, preferred_element_type=jnp.float32), LIMIT)
        up_act = jnp.clip(jnp.dot(expert_rows, up_block, preferred_element_type=jnp.float32), -LIMIT, LIMIT)
        hidden = ((up_act + 1.0) * gate_act * jax.nn.sigmoid(ALPHA * gate_act)).astype(jnp.bfloat16)
        pieces = hidden.reshape(EXPERT_ROWS, N_TP, FF_DEV).astype(jnp.float32)
        blocks = down_block.reshape(N_TP, FF_DEV, D).astype(jnp.float32)
        partial_sums = jnp.einsum('rnf,nfd->nrd', pieces, blocks).astype(jnp.bfloat16)
        return lax.optimization_barrier(jnp.sum(partial_sums.astype(jnp.float32), axis=0)).astype(jnp.bfloat16)
    expert_out = lax.map(expert, (buffer, gate_weight, up_weight, down_weight))
    picked = expert_out[routing, buffer_row].astype(jnp.float32)
    expert_mix = lax.optimization_barrier(jnp.sum(route_weight[:, :, None] * picked, axis=1))
    square_mean = lax.optimization_barrier(jnp.mean(expert_mix * expert_mix, axis=-1, keepdims=True))
    return (expert_mix * lax.rsqrt(square_mean + EPS) * out_gain).astype(jnp.bfloat16)
```

```python
import functools

import jax
import jax.numpy as jnp
from jax import lax
from jax.experimental import pallas as pl
from jax.experimental.pallas import tpu as pltpu
from jax.sharding import PartitionSpec as P

LIMIT = 7.0
ALPHA = 1.702
EPS = 1e-06
LANES = 128


def pack_kernel(tok_ref, route_ref, weight_ref, gain_ref, out_ref, *, half):
    width = tok_ref.shape[1]
    scaled = tok_ref[...].astype(jnp.float32)
    mean = jnp.mean(scaled * scaled, axis=-1, keepdims=True)
    out_ref[:, :width] = (scaled * lax.rsqrt(mean + EPS) * gain_ref[...]).astype(jnp.bfloat16)
    rows = tok_ref.shape[0]
    lane = lax.broadcasted_iota(jnp.int32, (rows, 2 * half), 1)
    expert = jnp.where(lane < half, lane, lane - half)
    dense = jnp.zeros((rows, 2 * half), jnp.float32)
    for k in range(route_ref.shape[1]):
        dense += jnp.where(route_ref[:, k : k + 1] == expert, weight_ref[:, k : k + 1], 0.0)
    high = dense.astype(jnp.bfloat16).astype(jnp.float32)
    out_ref[:, width:] = jnp.where(lane < half, high, dense - high).astype(jnp.bfloat16)


def pack(tokens, routing, route_weight, norm_gain, half):
    rows, width = tokens.shape
    return pl.pallas_call(
        functools.partial(pack_kernel, half=half),
        out_shape=jax.ShapeDtypeStruct((rows, width + 2 * half), jnp.bfloat16),
        name="pack",
    )(tokens, routing, route_weight, norm_gain.reshape(1, width))


def moe_kernel(place_ref, *refs, blocks, half, chunks):
    x_refs = refs[:blocks]
    gate_ref, up_ref, down_ref, keep_ref, send_ref, x_all, w_all, acc = refs[blocks:]
    step = pl.program_id(0)
    rows = x_refs[0].shape[0]
    width = x_all.shape[1]

    @pl.when(step == 0)
    def _():
        for b in range(blocks):
            x_all[b * rows : (b + 1) * rows, :] = x_refs[b][:, :width]
            w_all[b * rows : (b + 1) * rows, :] = x_refs[b][:, width:].astype(jnp.float32)

    expert = place_ref[0] + step // chunks
    lane = lax.broadcasted_iota(jnp.int32, w_all.shape, 1)
    mine = (lane == expert) | (lane == expert + half)
    weight = jnp.sum(jnp.where(mine, w_all[...], 0.0), axis=1, keepdims=True)
    x = x_all[...]
    gate = jnp.minimum(jnp.dot(x, gate_ref[0], preferred_element_type=jnp.float32), LIMIT)
    up = jnp.clip(jnp.dot(x, up_ref[0], preferred_element_type=jnp.float32), -LIMIT, LIMIT)
    hidden = ((up + 1.0) * gate * jax.nn.sigmoid(ALPHA * gate) * weight).astype(jnp.bfloat16)
    part = jnp.dot(hidden, down_ref[0], preferred_element_type=jnp.float32)

    @pl.when(step == 0)
    def _():
        acc[...] = part

    @pl.when(step > 0)
    def _():
        acc[...] += part

    @pl.when(step == pl.num_programs(0) - 1)
    def _():
        for b in range(blocks // 2):
            keep_ref[b] = acc[2 * b * rows : (2 * b + 1) * rows, :].astype(jnp.bfloat16)
            send_ref[b] = acc[(2 * b + 1) * rows : (2 * b + 2) * rows, :].astype(jnp.bfloat16)


def run_experts(x_blocks, gate_weight, up_weight, down_weight, place, half):
    blocks = len(x_blocks)
    rows, packed = x_blocks[0].shape
    experts, width, hidden = gate_weight.shape
    chunk = min(hidden, 256)
    chunks = hidden // chunk
    out = jax.ShapeDtypeStruct((blocks // 2, rows, width), jnp.bfloat16)
    whole = lambda shape: pl.BlockSpec(shape, lambda s, p: (0,) * len(shape))
    return pl.pallas_call(
        functools.partial(moe_kernel, blocks=blocks, half=half, chunks=chunks),
        grid_spec=pltpu.PrefetchScalarGridSpec(
            num_scalar_prefetch=1,
            grid=(experts * chunks,),
            in_specs=[whole((rows, packed))] * blocks
            + [
                pl.BlockSpec((1, width, chunk), lambda s, p: (s // chunks, 0, s % chunks)),
                pl.BlockSpec((1, width, chunk), lambda s, p: (s // chunks, 0, s % chunks)),
                pl.BlockSpec((1, chunk, width), lambda s, p: (s // chunks, s % chunks, 0)),
            ],
            out_specs=[whole(out.shape)] * 2,
            scratch_shapes=[
                pltpu.VMEM((blocks * rows, width), jnp.bfloat16),
                pltpu.VMEM((blocks * rows, 2 * half), jnp.float32),
                pltpu.VMEM((blocks * rows, width), jnp.float32),
            ],
        ),
        out_shape=[out, out],
        name="experts",
    )(place, *x_blocks, gate_weight, up_weight, down_weight)


def swap(value, axis, size, bit):
    return lax.ppermute(value, axis, [(s, s ^ bit) for s in range(size)])


def shift(value, axis, size, amount):
    return lax.ppermute(value, axis, [(s, (s + amount) % size) for s in range(size)])


def on_device(
    ep_size, tp_size,
    tokens, routing, route_weight, norm_gain, gate_weight, up_weight, down_weight, out_gain
):
    model_width = tokens.shape[1]
    local_experts = gate_weight.shape[0]
    all_experts = local_experts * ep_size
    half = -(-all_experts // 64) * 64
    ep_index = lax.axis_index("ep")
    tp_index = lax.axis_index("tp")
    bits = [1 << b for b in range(ep_size.bit_length() - 1)]

    arrived = {0: pack(tokens, routing, route_weight, norm_gain, half)}
    for bit in reversed(bits):
        for j in list(arrived):
            arrived[j ^ bit] = swap(arrived[j], "ep", ep_size, bit)
    x_blocks = [arrived[j] for j in range(ep_size)]
    place = (ep_index * local_experts).astype(jnp.int32).reshape(1)
    keep, send = run_experts(x_blocks, gate_weight, up_weight, down_weight, place, half)
    for bit in bits:
        got = swap(send, "ep", ep_size, bit)
        total = keep.astype(jnp.float32) + got.astype(jnp.float32)
        if bit == bits[-1]:
            mixed = total[0].astype(jnp.bfloat16)
        else:
            keep = total[0::2].astype(jnp.bfloat16)
            send = total[1::2].astype(jnp.bfloat16)
    out_width = model_width // tp_size
    block = lambda d: lax.dynamic_slice_in_dim(
        mixed, ((tp_index + d) % tp_size) * out_width, out_width, axis=1
    )
    expert_mix = block(0).astype(jnp.float32)
    for d in range(1, tp_size):
        expert_mix += shift(block(d), "tp", tp_size, d).astype(jnp.float32)
    square = jnp.sum(expert_mix * expert_mix, axis=1)
    square_sum = square
    for d in range(1, tp_size):
        square_sum += shift(square, "tp", tp_size, d)
    scale_factor = lax.rsqrt(square_sum / model_width + EPS)
    return (expert_mix * scale_factor[:, None] * out_gain).astype(jnp.bfloat16)


def solution(mesh):
    in_specs = (
        P(("grp", "ep"), None),
        P(("grp", "ep"), None),
        P(("grp", "ep"), None),
        P(),
        P("ep", None, "tp"),
        P("ep", None, "tp"),
        P("ep", "tp", None),
        P("tp"),
    )
    out_specs = P(("grp", "ep"), "tp")
    return jax.shard_map(
        functools.partial(on_device, mesh.shape["ep"], mesh.shape["tp"]),
        mesh=mesh, in_specs=in_specs, out_specs=out_specs, check_vma=False
    )
```

```python
import functools

import jax
import jax.numpy as jnp
from jax import lax
from jax.experimental import pallas as pl
from jax.experimental.pallas import tpu as pltpu
from jax.sharding import PartitionSpec as P


LIMIT = 7.0
ALPHA = 1.702
EPS = 1e-06


def pack_kernel(tok_ref, route_ref, weight_ref, gain_ref, out_ref, *, half):
    width = tok_ref.shape[1]
    scaled = tok_ref[...].astype(jnp.float32)
    mean = jnp.mean(scaled * scaled, axis=-1, keepdims=True)
    out_ref[:, :width] = (scaled * lax.rsqrt(mean + EPS) * gain_ref[...]).astype(jnp.bfloat16)
    rows = tok_ref.shape[0]
    line = lax.broadcasted_iota(jnp.int32, (2 * half, rows), 0)
    expert = jnp.where(line < half, line, line - half)
    dense = jnp.zeros((2 * half, rows), jnp.float32)
    for k in range(route_ref.shape[0]):
        dense += jnp.where(route_ref[k : k + 1, :] == expert, weight_ref[k : k + 1, :], 0.0)
    high = dense.astype(jnp.bfloat16).astype(jnp.float32)
    split = jnp.where(line < half, high, dense - high)
    out_ref[:, width:] = split.T.astype(jnp.bfloat16)


def pack(tokens, routing, route_weight, norm_gain, half):
    rows, width = tokens.shape
    return pl.pallas_call(
        functools.partial(pack_kernel, half=half),
        out_shape=jax.ShapeDtypeStruct((rows, width + 2 * half), jnp.bfloat16),
        compiler_params=pltpu.CompilerParams(vmem_limit_bytes=16 * 2**20),
        name="pack",
    )(tokens, routing.T, route_weight.T, norm_gain.reshape(1, width))


def moe_kernel(place_ref, *refs, blocks, half, chunk):
    x_refs = refs[:blocks]
    gate_ref, up_ref, down_ref, keep_ref, send_ref, x_all, w_all, acc = refs[blocks:]
    rows = x_refs[0].shape[0]
    width = x_all.shape[1]
    for b in range(blocks):
        x_all[b * rows : (b + 1) * rows, :] = x_refs[b][:, :width]
        w_all[b * rows : (b + 1) * rows, :] = x_refs[b][:, width:].astype(jnp.float32)
    lane = lax.broadcasted_iota(jnp.int32, w_all.shape, 1)
    for e in range(gate_ref.shape[0]):
        expert = place_ref[0] + e
        mine = (lane == expert) | (lane == expert + half)
        weight = jnp.sum(jnp.where(mine, w_all[...], 0.0), axis=1, keepdims=True)
        for c in range(0, gate_ref.shape[2], chunk):
            x = x_all[...]
            gate = jnp.dot(x, gate_ref[e, :, c : c + chunk], preferred_element_type=jnp.float32)
            up = jnp.dot(x, up_ref[e, :, c : c + chunk], preferred_element_type=jnp.float32)
            gate = jnp.minimum(gate, LIMIT)
            up = jnp.clip(up, -LIMIT, LIMIT)
            hidden = (up + 1.0) * gate * jax.nn.sigmoid(ALPHA * gate) * weight
            part = jnp.dot(
                hidden.astype(jnp.bfloat16), down_ref[e, c : c + chunk, :],
                preferred_element_type=jnp.float32,
            )
            if e == 0 and c == 0:
                acc[...] = part
            else:
                acc[...] += part
    for b in range(blocks // 2):
        keep_ref[b] = acc[2 * b * rows : (2 * b + 1) * rows, :].astype(jnp.bfloat16)
        send_ref[b] = acc[(2 * b + 1) * rows : (2 * b + 2) * rows, :].astype(jnp.bfloat16)


def fetch_kernel(*refs):
    count = (len(refs) - 2) // 2
    sources, targets, sems = refs[1 : 1 + count], refs[1 + count : -1], refs[-1]
    copies = [pltpu.make_async_copy(a, b, sems.at[i]) for i, (a, b) in enumerate(zip(sources, targets))]
    for copy in copies:
        copy.start()
    for copy in copies:
        copy.wait()


def fetch(after, weights):
    size = sum(w.size for w in weights)
    return pl.pallas_call(
        fetch_kernel,
        in_specs=[pl.BlockSpec(memory_space=pl.ANY)] * (1 + len(weights)),
        out_specs=[pl.BlockSpec(memory_space=pltpu.VMEM)] * len(weights),
        out_shape=[pltpu.VMEM(w.shape, w.dtype) for w in weights],
        scratch_shapes=[pltpu.SemaphoreType.DMA((len(weights),))],
        compiler_params=pltpu.CompilerParams(vmem_limit_bytes=16 * 2**20),
        cost_estimate=pl.CostEstimate(flops=256 * size, bytes_accessed=4 * size, transcendentals=0),
        name="fetch",
    )(after, *[pltpu.with_memory_space_constraint(w, pltpu.HBM) for w in weights])


def run_experts(x_blocks, gate_weight, up_weight, down_weight, place, half):
    blocks = len(x_blocks)
    rows = x_blocks[0].shape[0]
    width, hidden = gate_weight.shape[1:]
    out = jax.ShapeDtypeStruct((blocks // 2, rows, width), jnp.bfloat16)
    return pl.pallas_call(
        functools.partial(moe_kernel, blocks=blocks, half=half, chunk=min(hidden, 256)),
        in_specs=[pl.BlockSpec(memory_space=pltpu.SMEM)]
        + [pl.BlockSpec(memory_space=pltpu.VMEM)] * (blocks + 3),
        scratch_shapes=[
            pltpu.VMEM((blocks * rows, width), jnp.bfloat16),
            pltpu.VMEM((blocks * rows, 2 * half), jnp.float32),
            pltpu.VMEM((blocks * rows, width), jnp.float32),
        ],
        out_shape=[out, out],
        compiler_params=pltpu.CompilerParams(vmem_limit_bytes=40 * 2**20),
        name="experts",
    )(place, *x_blocks, *[pltpu.with_memory_space_constraint(w, pltpu.VMEM) for w in (gate_weight, up_weight, down_weight)])


def swap(value, axis, size, bit):
    return lax.ppermute(value, axis, [(s, s ^ bit) for s in range(size)])


def shift(value, axis, size, amount):
    return lax.ppermute(value, axis, [(s, (s + amount) % size) for s in range(size)])


def on_device(
    ep_size, tp_size,
    tokens, routing, route_weight, norm_gain, gate_weight, up_weight, down_weight, out_gain
):
    model_width = tokens.shape[1]
    local_experts = gate_weight.shape[0]
    all_experts = local_experts * ep_size
    half = -(-all_experts // 64) * 64
    ep_index = lax.axis_index("ep")
    tp_index = lax.axis_index("tp")
    bits = [1 << b for b in range(ep_size.bit_length() - 1)]

    place = (ep_index * local_experts).astype(jnp.int32).reshape(1)
    place, tokens = lax.optimization_barrier((place, tokens))
    packed = pack(tokens, routing, route_weight, norm_gain, half)
    weights = fetch(packed, (gate_weight, up_weight, down_weight))
    arrived = {0: packed, bits[-1]: swap(packed, "ep", ep_size, bits[-1])}
    for bit in reversed(bits[:-1]):
        for j in list(arrived):
            arrived[j ^ bit] = swap(arrived[j], "ep", ep_size, bit)
    x_blocks = [arrived[j] for j in range(ep_size)]
    keep, send = run_experts(x_blocks, *weights, place, half)
    for bit in bits:
        got = swap(send, "ep", ep_size, bit)
        total = keep.astype(jnp.float32) + got.astype(jnp.float32)
        if bit == bits[-1]:
            mixed = total[0].astype(jnp.bfloat16)
        else:
            keep = total[0::2].astype(jnp.bfloat16)
            send = total[1::2].astype(jnp.bfloat16)
    out_width = model_width // tp_size
    block = lambda d: lax.dynamic_slice_in_dim(
        mixed, ((tp_index + d) % tp_size) * out_width, out_width, axis=1
    )
    expert_mix = block(0).astype(jnp.float32)
    for d in range(1, tp_size):
        expert_mix += shift(block(d), "tp", tp_size, d).astype(jnp.float32)
    square = jnp.sum(expert_mix * expert_mix, axis=1)
    copies = jnp.broadcast_to(square, (tp_size,) + square.shape)
    square_sum = jnp.sum(lax.all_to_all(copies, "tp", 0, 0, tiled=True), axis=0)
    scale_factor = lax.rsqrt(square_sum / model_width + EPS)
    return (expert_mix * scale_factor[:, None] * out_gain).astype(jnp.bfloat16)


def solution(mesh):
    in_specs = (
        P(("grp", "ep"), None),
        P(("grp", "ep"), None),
        P(("grp", "ep"), None),
        P(),
        P("ep", None, "tp"),
        P("ep", None, "tp"),
        P("ep", "tp", None),
        P("tp"),
    )
    out_specs = P(("grp", "ep"), "tp")
    return jax.shard_map(
        functools.partial(on_device, mesh.shape["ep"], mesh.shape["tp"]),
        mesh=mesh, in_specs=in_specs, out_specs=out_specs, check_vma=False
    )
```

```python
import functools

import jax
import jax.numpy as jnp
from jax import lax
from jax.experimental import pallas as pl
from jax.experimental.pallas import tpu as pltpu
from jax.sharding import PartitionSpec as P


LIMIT = 7.0
ALPHA = 1.702
EPS = 1e-06


def pack_kernel(*refs, half):
    sources, out_ref, targets, sems = refs[:4], refs[4], refs[5:9], refs[9]
    copies = [pltpu.make_async_copy(a, b, sems.at[i]) for i, (a, b) in enumerate(zip(sources, targets))]
    for copy in copies:
        copy.start()
    for copy in copies:
        copy.wait()
    tok_ref, route_ref, weight_ref, gain_ref = targets
    width = tok_ref.shape[1]
    scaled = tok_ref[...].astype(jnp.float32)
    mean = jnp.mean(scaled * scaled, axis=-1, keepdims=True)
    out_ref[:, :width] = (scaled * lax.rsqrt(mean + EPS) * gain_ref[...]).astype(jnp.bfloat16)
    rows = tok_ref.shape[0]
    line = lax.broadcasted_iota(jnp.int32, (2 * half, rows), 0)
    expert = jnp.where(line < half, line, line - half)
    dense = jnp.zeros((2 * half, rows), jnp.float32)
    for k in range(route_ref.shape[0]):
        dense += jnp.where(route_ref[k : k + 1, :] == expert, weight_ref[k : k + 1, :], 0.0)
    high = dense.astype(jnp.bfloat16).astype(jnp.float32)
    split = jnp.where(line < half, high, dense - high)
    out_ref[:, width:] = split.T.astype(jnp.bfloat16)


def pack(tokens, routing, route_weight, norm_gain, half):
    rows, width = tokens.shape
    sources = (tokens, routing.T, route_weight.T, norm_gain.reshape(1, width))
    return pl.pallas_call(
        functools.partial(pack_kernel, half=half),
        in_specs=[pl.BlockSpec(memory_space=pl.ANY)] * len(sources),
        out_specs=pl.BlockSpec(memory_space=pltpu.VMEM),
        out_shape=jax.ShapeDtypeStruct((rows, width + 2 * half), jnp.bfloat16),
        scratch_shapes=[pltpu.VMEM(a.shape, a.dtype) for a in sources]
        + [pltpu.SemaphoreType.DMA((len(sources),))],
        compiler_params=pltpu.CompilerParams(vmem_limit_bytes=16 * 2**20),
        name="pack",
    )(*[pltpu.with_memory_space_constraint(a, pltpu.HBM) for a in sources])


def scale_kernel(mix_ref, gain_ref, out_ref):
    out_ref[...] = mix_ref[...] * gain_ref[...]


def scale(mix, gain):
    return pl.pallas_call(
        scale_kernel,
        out_shape=jax.ShapeDtypeStruct(mix.shape, jnp.float32),
        compiler_params=pltpu.CompilerParams(vmem_limit_bytes=8 * 2**20),
        cost_estimate=pl.CostEstimate(flops=2**26, bytes_accessed=8 * mix.size, transcendentals=0),
        name="scale",
    )(mix, gain.reshape(1, -1))


def moe_kernel(place_ref, *refs, blocks, half, chunk):
    x_refs = refs[:blocks]
    gate_ref, up_ref, down_ref, keep_ref, send_ref, x_all, w_all, acc = refs[blocks:]
    rows = x_refs[0].shape[0]
    width = x_all.shape[1]
    for b in range(blocks):
        x_all[b * rows : (b + 1) * rows, :] = x_refs[b][:, :width]
        w_all[b * rows : (b + 1) * rows, :] = x_refs[b][:, width:].astype(jnp.float32)
    lane = lax.broadcasted_iota(jnp.int32, w_all.shape, 1)
    for e in range(gate_ref.shape[0]):
        expert = place_ref[0] + e
        mine = (lane == expert) | (lane == expert + half)
        weight = jnp.sum(jnp.where(mine, w_all[...], 0.0), axis=1, keepdims=True)
        for c in range(0, gate_ref.shape[2], chunk):
            x = x_all[...]
            gate = jnp.dot(x, gate_ref[e, :, c : c + chunk], preferred_element_type=jnp.float32)
            up = jnp.dot(x, up_ref[e, :, c : c + chunk], preferred_element_type=jnp.float32)
            gate = jnp.minimum(gate, LIMIT)
            up = jnp.clip(up, -LIMIT, LIMIT)
            hidden = (up + 1.0) * gate * jax.nn.sigmoid(ALPHA * gate) * weight
            part = jnp.dot(
                hidden.astype(jnp.bfloat16), down_ref[e, c : c + chunk, :],
                preferred_element_type=jnp.float32,
            )
            if e == 0 and c == 0:
                acc[...] = part
            else:
                acc[...] += part
    for b in range(blocks // 2):
        keep_ref[b] = acc[2 * b * rows : (2 * b + 1) * rows, :].astype(jnp.bfloat16)
        send_ref[b] = acc[(2 * b + 1) * rows : (2 * b + 2) * rows, :].astype(jnp.bfloat16)


def fetch_kernel(*refs):
    count = (len(refs) - 2) // 2
    sources, targets, sems = refs[1 : 1 + count], refs[1 + count : -1], refs[-1]
    copies = [pltpu.make_async_copy(a, b, sems.at[i]) for i, (a, b) in enumerate(zip(sources, targets))]
    for copy in copies:
        copy.start()
    for copy in copies:
        copy.wait()


def fetch(after, weights):
    size = sum(w.size for w in weights)
    return pl.pallas_call(
        fetch_kernel,
        in_specs=[pl.BlockSpec(memory_space=pl.ANY)] * (1 + len(weights)),
        out_specs=[pl.BlockSpec(memory_space=pltpu.VMEM)] * len(weights),
        out_shape=[pltpu.VMEM(w.shape, w.dtype) for w in weights],
        scratch_shapes=[pltpu.SemaphoreType.DMA((len(weights),))],
        compiler_params=pltpu.CompilerParams(vmem_limit_bytes=16 * 2**20),
        cost_estimate=pl.CostEstimate(flops=256 * size, bytes_accessed=4 * size, transcendentals=0),
        name="fetch",
    )(after, *[pltpu.with_memory_space_constraint(w, pltpu.HBM) for w in weights])


def run_experts(x_blocks, gate_weight, up_weight, down_weight, place, half):
    blocks = len(x_blocks)
    rows = x_blocks[0].shape[0]
    width, hidden = gate_weight.shape[1:]
    out = pltpu.VMEM((blocks // 2, rows, width), jnp.bfloat16)
    return pl.pallas_call(
        functools.partial(moe_kernel, blocks=blocks, half=half, chunk=min(hidden, 256)),
        in_specs=[pl.BlockSpec(memory_space=pltpu.SMEM)]
        + [pl.BlockSpec(memory_space=pltpu.VMEM)] * (blocks + 3),
        scratch_shapes=[
            pltpu.VMEM((blocks * rows, width), jnp.bfloat16),
            pltpu.VMEM((blocks * rows, 2 * half), jnp.float32),
            pltpu.VMEM((blocks * rows, width), jnp.float32),
        ],
        out_shape=[out, out],
        compiler_params=pltpu.CompilerParams(vmem_limit_bytes=40 * 2**20),
        name="experts",
    )(place, *x_blocks, *[pltpu.with_memory_space_constraint(w, pltpu.VMEM) for w in (gate_weight, up_weight, down_weight)])


def swap(value, axis, size, bit):
    return lax.ppermute(value, axis, [(s, s ^ bit) for s in range(size)])


def shift(value, axis, size, amount):
    return lax.ppermute(value, axis, [(s, (s + amount) % size) for s in range(size)])


def on_device(
    ep_size, tp_size,
    tokens, routing, route_weight, norm_gain, gate_weight, up_weight, down_weight, out_gain
):
    model_width = tokens.shape[1]
    local_experts = gate_weight.shape[0]
    all_experts = local_experts * ep_size
    half = -(-all_experts // 64) * 64
    ep_index = lax.axis_index("ep")
    tp_index = lax.axis_index("tp")
    bits = [1 << b for b in range(ep_size.bit_length() - 1)]

    place = (ep_index * local_experts).astype(jnp.int32).reshape(1)
    place, tokens = lax.optimization_barrier((place, tokens))
    packed = pack(tokens, routing, route_weight, norm_gain, half)
    weights = fetch(packed, (gate_weight, up_weight, down_weight))
    arrived = {0: packed, bits[-1]: swap(packed, "ep", ep_size, bits[-1])}
    for bit in reversed(bits[:-1]):
        for j in list(arrived):
            arrived[j ^ bit] = swap(arrived[j], "ep", ep_size, bit)
    x_blocks = [arrived[j] for j in range(ep_size)]
    keep, send = run_experts(x_blocks, *weights, place, half)
    for bit in bits:
        got = swap(send, "ep", ep_size, bit)
        total = keep.astype(jnp.float32) + got.astype(jnp.float32)
        if bit == bits[-1]:
            mixed = total[0].astype(jnp.bfloat16)
        else:
            keep = total[0::2].astype(jnp.bfloat16)
            send = total[1::2].astype(jnp.bfloat16)
    out_width = model_width // tp_size
    block = lambda d: lax.dynamic_slice_in_dim(
        mixed, ((tp_index + d) % tp_size) * out_width, out_width, axis=1
    )
    expert_mix = block(0).astype(jnp.float32)
    for d in range(1, tp_size):
        expert_mix += shift(block(d), "tp", tp_size, d).astype(jnp.float32)
    square = jnp.sum(expert_mix * expert_mix, axis=1)
    copies = jnp.broadcast_to(square, (tp_size,) + square.shape)
    square_sum = jnp.sum(lax.all_to_all(copies, "tp", 0, 0), axis=0)
    scaled = scale(expert_mix, out_gain)
    scale_factor = lax.rsqrt(square_sum / model_width + EPS)
    return (scaled * scale_factor[:, None]).astype(jnp.bfloat16)


def solution(mesh):
    in_specs = (
        P(("grp", "ep"), None),
        P(("grp", "ep"), None),
        P(("grp", "ep"), None),
        P(),
        P("ep", None, "tp"),
        P("ep", None, "tp"),
        P("ep", "tp", None),
        P("tp"),
    )
    out_specs = P(("grp", "ep"), "tp")
    return jax.shard_map(
        functools.partial(on_device, mesh.shape["ep"], mesh.shape["tp"]),
        mesh=mesh, in_specs=in_specs, out_specs=out_specs, check_vma=False
    )
```

```python
import functools

import jax
import jax.numpy as jnp
from jax import lax
from jax.experimental import pallas as pl
from jax.experimental.pallas import tpu as pltpu
from jax.sharding import PartitionSpec as P


LIMIT = 7.0
ALPHA = 1.702
EPS = 1e-06


def pack_kernel(*refs, half):
    sources, out_ref, targets, sems = refs[:4], refs[4], refs[5:9], refs[9]
    copies = [pltpu.make_async_copy(a, b, sems.at[i]) for i, (a, b) in enumerate(zip(sources, targets))]
    for copy in copies:
        copy.start()
    for copy in copies:
        copy.wait()
    tok_ref, route_ref, weight_ref, gain_ref = targets
    width = tok_ref.shape[1]
    scaled = tok_ref[...].astype(jnp.float32)
    mean = jnp.mean(scaled * scaled, axis=-1, keepdims=True)
    out_ref[:, :width] = (scaled * lax.rsqrt(mean + EPS) * gain_ref[...]).astype(jnp.bfloat16)
    rows = tok_ref.shape[0]
    line = lax.broadcasted_iota(jnp.int32, (2 * half, rows), 0)
    expert = jnp.where(line < half, line, line - half)
    dense = jnp.zeros((2 * half, rows), jnp.float32)
    for k in range(route_ref.shape[0]):
        dense += jnp.where(route_ref[k : k + 1, :] == expert, weight_ref[k : k + 1, :], 0.0)
    high = dense.astype(jnp.bfloat16).astype(jnp.float32)
    split = jnp.where(line < half, high, dense - high)
    out_ref[:, width:] = split.T.astype(jnp.bfloat16)


def pack(tokens, routing, route_weight, norm_gain, half):
    rows, width = tokens.shape
    sources = (tokens, routing.T, route_weight.T, norm_gain.reshape(1, width))
    return pl.pallas_call(
        functools.partial(pack_kernel, half=half),
        in_specs=[pl.BlockSpec(memory_space=pl.ANY)] * len(sources),
        out_specs=pl.BlockSpec(memory_space=pltpu.VMEM),
        out_shape=jax.ShapeDtypeStruct((rows, width + 2 * half), jnp.bfloat16),
        scratch_shapes=[pltpu.VMEM(a.shape, a.dtype) for a in sources]
        + [pltpu.SemaphoreType.DMA((len(sources),))],
        compiler_params=pltpu.CompilerParams(vmem_limit_bytes=16 * 2**20),
        name="pack",
    )(*[pltpu.with_memory_space_constraint(a, pltpu.HBM) for a in sources])


def moe_kernel(place_ref, *refs, blocks, half):
    x_refs = refs[:blocks]
    gate_ref, up_ref, down_ref, keep_ref, send_ref, x_all, w_all, hidden_all = refs[blocks:]
    rows = x_refs[0].shape[0]
    width = x_all.shape[1]
    experts, _, size = gate_ref.shape
    for b in range(blocks):
        x_all[b * rows : (b + 1) * rows, :] = x_refs[b][:, :width]
        w_all[b * rows : (b + 1) * rows, :] = x_refs[b][:, width:].astype(jnp.float32)
    lane = lax.broadcasted_iota(jnp.int32, w_all.shape, 1)
    for e in range(experts):
        expert = place_ref[0] + e
        mine = (lane == expert) | (lane == expert + half)
        weight = jnp.sum(jnp.where(mine, w_all[...], 0.0), axis=1, keepdims=True)
        x = x_all[...]
        gate = jnp.minimum(jnp.dot(x, gate_ref[e], preferred_element_type=jnp.float32), LIMIT)
        up = jnp.clip(jnp.dot(x, up_ref[e], preferred_element_type=jnp.float32), -LIMIT, LIMIT)
        hidden = (up + 1.0) * gate * jax.nn.sigmoid(ALPHA * gate) * weight
        hidden_all[:, e * size : (e + 1) * size] = hidden.astype(jnp.bfloat16)
    for n in range(0, width, 512):
        down = down_ref[:, :, n : n + 512].reshape(experts * size, 512)
        part = jnp.dot(hidden_all[...], down, preferred_element_type=jnp.float32)
        part = part.astype(jnp.bfloat16)
        for b in range(blocks // 2):
            keep_ref[b, :, n : n + 512] = part[2 * b * rows : (2 * b + 1) * rows, :]
            send_ref[b, :, n : n + 512] = part[(2 * b + 1) * rows : (2 * b + 2) * rows, :]


def run_experts(x_blocks, weights, place, half):
    blocks = len(x_blocks)
    rows = x_blocks[0].shape[0]
    experts, width, hidden = weights[0].shape
    out = pltpu.VMEM((blocks // 2, rows, width), jnp.bfloat16)
    return pl.pallas_call(
        functools.partial(moe_kernel, blocks=blocks, half=half),
        in_specs=[pl.BlockSpec(memory_space=pltpu.SMEM)]
        + [pl.BlockSpec(memory_space=pltpu.VMEM)] * (blocks + 3),
        scratch_shapes=[
            pltpu.VMEM((blocks * rows, width), jnp.bfloat16),
            pltpu.VMEM((blocks * rows, 2 * half), jnp.float32),
            pltpu.VMEM((blocks * rows, experts * hidden), jnp.bfloat16),
        ],
        out_shape=[out, out],
        compiler_params=pltpu.CompilerParams(vmem_limit_bytes=20 * 2**20),
        name="experts",
    )(place, *x_blocks, *[pltpu.with_memory_space_constraint(w, pltpu.VMEM) for w in weights])


def fetch_kernel(*refs):
    count = (len(refs) - 2) // 2
    sources, targets, sems = refs[1 : 1 + count], refs[1 + count : -1], refs[-1]
    copies = [pltpu.make_async_copy(a, b, sems.at[i]) for i, (a, b) in enumerate(zip(sources, targets))]
    for copy in copies:
        copy.start()
    for copy in copies:
        copy.wait()


def fetch(after, weights):
    size = sum(w.size for w in weights)
    return pl.pallas_call(
        fetch_kernel,
        in_specs=[pl.BlockSpec(memory_space=pl.ANY)] * (1 + len(weights)),
        out_specs=[pl.BlockSpec(memory_space=pltpu.VMEM)] * len(weights),
        out_shape=[pltpu.VMEM(w.shape, w.dtype) for w in weights],
        scratch_shapes=[pltpu.SemaphoreType.DMA((len(weights),))],
        compiler_params=pltpu.CompilerParams(vmem_limit_bytes=16 * 2**20),
        cost_estimate=pl.CostEstimate(flops=256 * size, bytes_accessed=4 * size, transcendentals=0),
        name="fetch",
    )(after, *[pltpu.with_memory_space_constraint(w, pltpu.HBM) for w in weights])


def swap(value, axis, size, bit):
    return lax.ppermute(value, axis, [(s, s ^ bit) for s in range(size)])


def shift(value, axis, size, amount):
    return lax.ppermute(value, axis, [(s, (s + amount) % size) for s in range(size)])


def on_device(
    ep_size, tp_size,
    tokens, routing, route_weight, norm_gain, gate_weight, up_weight, down_weight, out_gain
):
    model_width = tokens.shape[1]
    local_experts = gate_weight.shape[0]
    all_experts = local_experts * ep_size
    half = -(-all_experts // 64) * 64
    ep_index = lax.axis_index("ep")
    tp_index = lax.axis_index("tp")
    bits = [1 << b for b in range(ep_size.bit_length() - 1)]

    place = (ep_index * local_experts).astype(jnp.int32).reshape(1)
    place, tokens = lax.optimization_barrier((place, tokens))
    packed = pack(tokens, routing, route_weight, norm_gain, half)
    weights = fetch(packed, (gate_weight, up_weight, down_weight))
    arrived = {0: packed, bits[-1]: swap(packed, "ep", ep_size, bits[-1])}
    for bit in reversed(bits[:-1]):
        for j in list(arrived):
            arrived[j ^ bit] = swap(arrived[j], "ep", ep_size, bit)
    x_blocks = [arrived[j] for j in range(ep_size)]
    keep, send = run_experts(x_blocks, weights, place, half)
    for bit in bits:
        got = swap(send, "ep", ep_size, bit)
        total = keep.astype(jnp.float32) + got.astype(jnp.float32)
        if bit == bits[-1]:
            mixed = total[0].astype(jnp.bfloat16)
        else:
            keep = total[0::2].astype(jnp.bfloat16)
            send = total[1::2].astype(jnp.bfloat16)
    out_width = model_width // tp_size
    block = lambda d: lax.dynamic_slice_in_dim(
        mixed, ((tp_index + d) % tp_size) * out_width, out_width, axis=1
    )
    expert_mix = block(0).astype(jnp.float32)
    for d in range(1, tp_size):
        expert_mix += shift(block(d), "tp", tp_size, d).astype(jnp.float32)
    square = jnp.sum(expert_mix * expert_mix, axis=1)
    square_sum = square
    for bit in (1 << b for b in range(tp_size.bit_length() - 1)):
        square_sum += swap(square_sum, "tp", tp_size, bit)
    scale_factor = lax.rsqrt(square_sum / model_width + EPS)
    return (expert_mix * scale_factor[:, None] * out_gain).astype(jnp.bfloat16)


def solution(mesh):
    in_specs = (
        P(("grp", "ep"), None),
        P(("grp", "ep"), None),
        P(("grp", "ep"), None),
        P(),
        P("ep", None, "tp"),
        P("ep", None, "tp"),
        P("ep", "tp", None),
        P("tp"),
    )
    out_specs = P(("grp", "ep"), "tp")
    return jax.shard_map(
        functools.partial(on_device, mesh.shape["ep"], mesh.shape["tp"]),
        mesh=mesh, in_specs=in_specs, out_specs=out_specs, check_vma=False
    )
```
